32 devices in a mesh: sp: 8 (over z, core), tp: 4 (over y, x).
Axes of the slice: x: 2, y: 2, z: 4, core: 2. Of those that a mesh axis runs over, the one named last changes fastest.
Arguments:
- cotangent: bfloat16 [1024, 2048], P('sp'), may hold values from -6 to 6
- mixer_sum: bfloat16 [1024, 2048], P('sp'), may hold values from -180 to 180
- ffn_gain: float32 [2048], replicated, may hold values from 0.1 to 1.9
- expert_ids: int32 [1024, 2], P('sp'), may hold values from 0 to 7, all different within a row; in each aligned block of 128 rows (0 to 127, 128 to 255, ...) at most 40 rows name the same one
- route_weight: float32 [1024, 2], P('sp'), may hold values from 0.1 to 1
- gate_weights: bfloat16 [8, 2048, 2048], P('sp', None, 'tp'), may hold values from -0.125 to 0.125
- up_weights: bfloat16 [8, 2048, 2048], P('sp', None, 'tp'), may hold values from -0.125 to 0.125
- down_weights: bfloat16 [8, 2048, 2048], P('sp', 'tp'), may hold values from -0.125 to 0.125
- out_weight: bfloat16 [2048, 1024], P(None, 'tp'), may hold values from -5 to 5
- conv_output: bfloat16 [1024, 1024], P('sp', 'tp'), may hold values from -6 to 6
- norm_mean: float32 [1024], P('sp'), may hold values from -3 to 3
- norm_rstd: float32 [1024], P('sp'), may hold values from 0.5 to 2
- norm_gain: float32 [1024], P('tp'), may hold values from 0.1 to 1.9
- conv_taps: float32 [31, 1024], P(None, 'tp'), may hold values from -1 to 1
- conv_value: bfloat16 [1024, 1024], P('sp', 'tp'), may hold values from -6 to 6
- conv_gate: bfloat16 [1024, 1024], P('sp', 'tp'), may hold values from -6 to 6
Outputs:
- grad_gate_weights: bfloat16 [8, 2048, 2048], P('sp', None, 'tp')
- grad_up_weights: bfloat16 [8, 2048, 2048], P('sp', None, 'tp')
- grad_down_weights: bfloat16 [8, 2048, 2048], P('sp', 'tp')
- grad_out_weight: float32 [2048, 1024], P('sp', 'tp')
- grad_conv_value: bfloat16 [1024, 1024], P('sp', 'tp')
- grad_conv_gate: bfloat16 [1024, 1024], P('sp', 'tp')
The draws below stay inside these ranges and needn't reach their ends.
Inputs may be any that keep to these rules, and one draw needn't show every extreme that they name: `expert_ids`: the 2 experts of a row differ. Among the rows of one index of sp no expert is named more than 40 times, and in every draw some index names some expert exactly 40 times.
All inputs are finite; a program needn't handle non-finite values.
Results may differ from the reference program's by a relative error of at most 0.024.
Values may be sent and summed in bfloat16 or wider, within the bound.
A program may use at most 64 MiB of HBM per device.

```python
import math
import jax
import jax.numpy as jnp
import numpy as np
from jax import lax

D = 2048
CONV = 1024
FF = 2048
KW = 31
TOP = 2
TOK_DEV = 128
SEQ = 1024
EXPERTS = 8
CAP = 40
N_SP = 8
N_TP = 4


def draw_mixer_sum(key, part):
    base_key = jax.random.fold_in(key, 11)
    first, second, third = jax.random.split(base_key, 3)
    column_scale = jnp.exp(jax.random.uniform(second, (1, D), jnp.float32, 0.0, jnp.log(10.0)))
    row_scale = jnp.exp(jax.random.uniform(third, (SEQ, 1), jnp.float32, jnp.log(0.3), jnp.log(3.0)))
    values = jnp.clip(jax.random.normal(first, (SEQ, D), jnp.float32), -6.0, 6.0)
    return (values * column_scale * row_scale).astype(jnp.bfloat16)


def draw_out_weight(key, part):
    base_key = jax.random.fold_in(key, 23)
    first, second = jax.random.split(base_key, 2)
    rising = jnp.exp(jnp.log(3.0) * jnp.arange(CONV, dtype=jnp.float32) / CONV)[None, :]
    common = jnp.clip(jax.random.normal(second, (D, 1), jnp.float32), -6.0, 6.0)
    values = jnp.clip(jax.random.normal(first, (D, CONV), jnp.float32), -6.0, 6.0) + common
    return (values * rising / jnp.sqrt(2.0 * D)).astype(jnp.bfloat16)


def with_spikes(result, rng, source, target, parts, factor):
    def block_of(axis_at):
        return (jnp.arange(result.shape[axis_at]) // (result.shape[axis_at] // parts)).reshape((-1,) + (1,) * (result.ndim - 1 - axis_at))

    near = jax.random.permutation(rng, parts)[block_of(target)]
    second = (block_of(target) + parts // 2) % parts
    return jnp.where((block_of(source) == near) | (block_of(source) == second), factor * result, result)


def block_levels(rng, dims, shards, least, largest):
    def one(position, parts):
        draws = jax.random.uniform(jax.random.fold_in(jax.random.fold_in(rng, 6), position), (parts,), jnp.float32, least / len(shards), largest / len(shards))
        return jnp.repeat(jnp.exp(draws), dims[position] // parts).reshape((-1,) + (1,) * (len(dims) - position - 1))

    level = one(*shards[0])
    for cut in shards[1:]:
        level = level * one(*cut)
    return level


def deal_out(own_key, own, number, rows, number_of, top, reach, slope):
    sequence = jax.random.permutation(own_key, number_of)
    crowded, ordinary = portions_of(number_of, rows * top, reach, slope, True), portions_of(number_of, rows * top, reach, slope, False)
    places = jnp.arange(number_of)

    def named(sizes, offset_by):
        used = int((sizes > 0).sum())
        fixed = max(1, used // 4)
        passed = fixed + (places - fixed + offset_by * (used - fixed)) % max(1, number_of - fixed)
        return jnp.zeros((number_of,), jnp.int32).at[sequence[jnp.where(places < fixed, places, passed)]].set(jnp.asarray(sizes, jnp.int32))

    sizes = jnp.where(number % 4 == 0, named(crowded, number // 4), named(ordinary, number - number // 4 - 1))
    mixed = jax.random.permutation(jax.random.fold_in(own, 3), number_of)
    giver, receiver = mixed[0:number_of // 2 * 2:2], mixed[1:number_of // 2 * 2:2]
    slack = jnp.minimum(sizes[giver] - 1, reach - sizes[receiver]) // 2
    slack = jnp.where((giver == sequence[0]) | (receiver == sequence[0]) | (sizes[receiver] == 0), 0, jnp.maximum(slack, 0))
    passed = jax.random.randint(jax.random.fold_in(own, 4), (number_of // 2,), 0, 1 << 20) % (slack + 1)
    sizes = sizes.at[giver].add(-passed).at[receiver].add(passed)
    items = jnp.searchsorted(jnp.cumsum(sizes), jnp.arange(rows * top), side="right").astype(jnp.int32)
    table = items.reshape(top, rows).T
    table = table[jax.random.permutation(jax.random.fold_in(own, 1), rows)]
    offset_by = jax.random.randint(jax.random.fold_in(own, 2), (rows, 1), 0, top)
    return jnp.take_along_axis(table, (jnp.arange(top)[None, :] + offset_by) % top, axis=1)


def portions_of(number_of, total, reach, lean, full):
    loads = [(1 << 20) // math.isqrt(standing ** lean) + 1 for standing in range(1, number_of + 1)]
    largest = reach if full else min(reach, max(-(-total // number_of), total * loads[0] // sum(loads)))
    least = 1 if total - largest >= number_of - 1 else 0
    holding, surplus = [largest] + [least] * (number_of - 1), total - largest - least * (number_of - 1)
    while surplus > 0:
        movable = [i for i in range(1, number_of) if holding[i] < largest] or [i for i in range(1, number_of) if holding[i] < reach]
        mass, budget = sum([loads[i] for i in movable]), surplus
        for i in movable:
            addition = min(reach - holding[i], max(1, budget * loads[i] // mass), surplus)
            holding[i] = holding[i] + addition
            surplus = surplus - addition
    return np.array(holding)


def normal_values(rng, shape, spread, reach, pieces=(), kind=jnp.bfloat16):
    factor_of = block_levels(rng, shape, pieces, -0.22, 0.18) if pieces else 1.0
    result = jax.random.normal(rng, shape, jnp.float32) * spread * factor_of
    return jnp.minimum(jnp.maximum(result, -reach), reach).astype(kind)


def gaussian_with(key, shape, deviation, limit, cuts, heavy, held_as=jnp.bfloat16):
    values = deviation * jax.random.normal(key, shape, jnp.float32)
    if cuts:
        values = values * block_levels(key, shape, cuts, -0.22, 0.18)
    return jnp.clip(with_spikes(values, jax.random.fold_in(key, 3), *heavy), -limit, limit).astype(held_as)


def setup_inputs(seed: int = 0) -> dict:
    key_of = jax.random.split(jax.random.key(seed), 17)
    cotangent = gaussian_with(key_of[0], (SEQ, D), 1.0, 6.0, ((0, 8),), (0, 1, 8, 2.0))
    mixer_sum = draw_mixer_sum(jax.random.fold_in(key_of[16], 71), 0)
    ffn_gain = jnp.clip(1.0 + 0.18 * jax.random.normal(key_of[2], (D,), jnp.float32), 0.1, 1.9)
    expert_ids_keys = jax.random.split(jax.random.fold_in(key_of[3], 1), SEQ // TOK_DEV)
    expert_ids_turns = jax.random.permutation(jax.random.fold_in(key_of[3], 3), SEQ // TOK_DEV)
    expert_ids = jax.vmap(lambda own, number: deal_out(jax.random.fold_in(key_of[3], 2), own, number, TOK_DEV, EXPERTS, TOP, CAP, 1))(expert_ids_keys, expert_ids_turns).reshape((SEQ, TOP))
    route_weight = jnp.clip(0.1 + 0.9 * jax.random.uniform(key_of[4], (SEQ, TOP), jnp.float32) ** block_levels(key_of[4], (SEQ, TOP), ((0, 8),), -0.2, 0.2), 0.1, 1.0)
    gate_weights = normal_values(key_of[5], (EXPERTS, D, FF), D ** -0.5, 0.125, ((0, 8), (2, 4)))
    up_weights = normal_values(key_of[6], (EXPERTS, D, FF), D ** -0.5, 0.125, ((0, 8), (2, 4)))
    down_weights = normal_values(key_of[7], (EXPERTS, FF, D), FF ** -0.5, 0.125, ((0, 8), (1, 4)))
    out_weight = draw_out_weight(jax.random.fold_in(key_of[16], 71), 0)
    conv_output = normal_values(key_of[9], (SEQ, CONV), 1.0, 6.0, ((0, 8), (1, 4)))
    norm_mean = normal_values(key_of[10], (SEQ,), 0.5, 3.0, ((0, 8),), jnp.float32)
    norm_rstd = jnp.clip(jnp.exp(math.log(2.0) - 1.3862944 * jax.random.uniform(key_of[11], (SEQ,), jnp.float32) ** block_levels(key_of[11], (SEQ,), ((0, 8),), -0.2, 0.2)), 0.5, 2.0)
    norm_gain = jnp.clip(1.0 + 0.18 * jax.random.normal(key_of[12], (CONV,), jnp.float32), 0.1, 1.9)
    conv_taps = normal_values(key_of[13], (KW, CONV), KW ** -0.5, 1.0, ((1, 4),), jnp.float32)
    conv_value = normal_values(key_of[14], (SEQ, CONV), 1.0, 6.0, ((0, 8), (1, 4)))
    conv_gate = normal_values(key_of[15], (SEQ, CONV), 1.5, 6.0, ((0, 8), (1, 4)))
    return {"cotangent": cotangent, "mixer_sum": mixer_sum, "ffn_gain": ffn_gain, "expert_ids": expert_ids, "route_weight": route_weight, "gate_weights": gate_weights, "up_weights": up_weights, "down_weights": down_weights, "out_weight": out_weight, "conv_output": conv_output, "norm_mean": norm_mean, "norm_rstd": norm_rstd, "norm_gain": norm_gain, "conv_taps": conv_taps, "conv_value": conv_value, "conv_gate": conv_gate}


epsilon = 1e-06

def slot_layout(route_ids, capacity, expert_count):
    flat_ids = route_ids.reshape(-1).astype(jnp.int32)
    onehot = (flat_ids[:, None] == jnp.arange(expert_count, dtype=jnp.int32)[None, :]).astype(jnp.int32)
    earlier = jnp.cumsum(onehot, axis=0) - onehot
    places = lax.optimization_barrier(jnp.sum(earlier * onehot, axis=1))
    return (flat_ids * capacity + places).astype(jnp.int32)

def slot_sources(entry_slot, slot_count):
    matches = entry_slot[None, :] == jnp.arange(slot_count, dtype=jnp.int32)[:, None]
    filled = jnp.any(matches, axis=1)
    entries = jnp.arange(entry_slot.shape[0], dtype=jnp.int32)
    sources = lax.optimization_barrier(jnp.sum(jnp.where(matches, entries[None, :], 0), axis=1)).astype(jnp.int32)
    return (sources, filled)

def reference(cotangent, mixer_sum, ffn_gain, expert_ids, route_weight, gate_weights, up_weights, down_weights, out_weight, conv_output, norm_mean, norm_rstd, norm_gain, conv_taps, conv_value, conv_gate):
    mixed_float = mixer_sum.astype(jnp.float32)
    row_rstd = lax.rsqrt(lax.optimization_barrier(jnp.mean(mixed_float * mixed_float, axis=1, keepdims=True)) + epsilon)
    mixer_hat = mixed_float * row_rstd
    normed = (mixer_hat * ffn_gain).astype(jnp.bfloat16)
    scaled = (route_weight[:, :, None] * cotangent.astype(jnp.float32)[:, None, :]).astype(jnp.bfloat16)
    normed_blocks = normed.reshape(N_SP, TOK_DEV, D)
    scaled_blocks = scaled.reshape(N_SP, TOK_DEV * TOP, D)
    id_blocks = expert_ids.reshape(N_SP, TOK_DEV, TOP)

    def build(id_block, normed_block, scaled_block):
        entry_slot = slot_layout(id_block, CAP, EXPERTS)
        sources, filled = slot_sources(entry_slot, EXPERTS * CAP)
        zero_row = jnp.zeros((), jnp.bfloat16)
        rows_out = jnp.where(filled[:, None], normed_block[sources // TOP], zero_row)
        cots_out = jnp.where(filled[:, None], scaled_block[sources], zero_row)
        return (rows_out, cots_out, entry_slot)
    rows_all, cots_all, slots_all = jax.vmap(build)(id_blocks, normed_blocks, scaled_blocks)
    expert_rows = rows_all.reshape(N_SP, EXPERTS, CAP, D).transpose(1, 0, 2, 3).reshape(EXPERTS, N_SP * CAP, D)
    expert_cots = cots_all.reshape(N_SP, EXPERTS, CAP, D).transpose(1, 0, 2, 3).reshape(EXPERTS, N_SP * CAP, D)
    share_units = FF // N_TP
    row_total = N_SP * CAP

    def expert_backward(packed):
        rows_in, cots_in, gate_mat, up_mat, down_mat = packed
        gate_pre = jnp.dot(rows_in, gate_mat, preferred_element_type=jnp.float32)
        up_pre = jnp.dot(rows_in, up_mat, preferred_element_type=jnp.float32)
        gate_sig = jax.nn.sigmoid(gate_pre)
        active = gate_pre * gate_sig
        hidden = (active * up_pre).astype(jnp.bfloat16)
        d_hidden = jnp.dot(cots_in, down_mat.T, preferred_element_type=jnp.float32)
        d_gate = (d_hidden * up_pre * gate_sig * (1.0 + gate_pre * (1.0 - gate_sig))).astype(jnp.bfloat16)
        d_up = (d_hidden * active).astype(jnp.bfloat16)
        grad_down = jnp.dot(hidden.T, cots_in, preferred_element_type=jnp.float32).astype(jnp.bfloat16)
        grad_gate = jnp.dot(rows_in.T, d_gate, preferred_element_type=jnp.float32).astype(jnp.bfloat16)
        grad_up = jnp.dot(rows_in.T, d_up, preferred_element_type=jnp.float32).astype(jnp.bfloat16)
        gate_split = d_gate.astype(jnp.float32).reshape(row_total, N_TP, share_units)
        up_split = d_up.astype(jnp.float32).reshape(row_total, N_TP, share_units)
        gate_wsplit = gate_mat.astype(jnp.float32).reshape(D, N_TP, share_units)
        up_wsplit = up_mat.astype(jnp.float32).reshape(D, N_TP, share_units)
        partial_value = jnp.einsum('rjf,djf->jrd', gate_split, gate_wsplit) + jnp.einsum('rjf,djf->jrd', up_split, up_wsplit)
        rounded = lax.optimization_barrier(partial_value.astype(jnp.bfloat16)).astype(jnp.float32)
        back_rows = lax.optimization_barrier(jnp.sum(rounded, axis=0)).astype(jnp.bfloat16)
        return (grad_gate, grad_up, grad_down, back_rows)
    grad_gate_weights, grad_up_weights, grad_down_weights, back_all = lax.map(expert_backward, (expert_rows, expert_cots, gate_weights, up_weights, down_weights))
    returned = back_all.reshape(EXPERTS, N_SP, CAP, D).transpose(1, 0, 2, 3).reshape(N_SP, EXPERTS * CAP, D)

    def pick_back(buffer_rows, slot_index):
        return buffer_rows[slot_index]
    picked = jax.vmap(pick_back)(returned, slots_all)
    d_normed = lax.optimization_barrier(jnp.sum(picked.astype(jnp.float32).reshape(SEQ, TOP, D), axis=1))
    d_hat = d_normed * ffn_gain
    d_mixed = cotangent.astype(jnp.float32) + row_rstd * (d_hat - mixer_hat * lax.optimization_barrier(jnp.mean(d_hat * mixer_hat, axis=1, keepdims=True)))
    d_mixed_b = d_mixed.astype(jnp.bfloat16)
    norm_in = (conv_output.astype(jnp.float32) - norm_mean[:, None]) * norm_rstd[:, None]
    norm_scaled = norm_in * norm_gain
    norm_sig = jax.nn.sigmoid(norm_scaled)
    conv_act = (norm_scaled * norm_sig).astype(jnp.bfloat16)
    grad_out_weight = jnp.dot(d_mixed_b.T, conv_act, preferred_element_type=jnp.float32)
    d_act = jnp.dot(d_mixed_b, out_weight, preferred_element_type=jnp.float32)
    d_in = d_act * norm_sig * (1.0 + norm_scaled * (1.0 - norm_sig)) * norm_gain
    d_conv = norm_rstd[:, None] * (d_in - lax.optimization_barrier(jnp.mean(d_in, axis=1, keepdims=True)) - norm_in * lax.optimization_barrier(jnp.mean(d_in * norm_in, axis=1, keepdims=True)))
    padded = jnp.pad(d_conv, ((0, KW - 1), (0, 0)))
    d_mixin = jnp.zeros((SEQ, CONV), jnp.float32)
    for tap_index in range(KW):
        d_mixin = d_mixin + conv_taps[tap_index] * padded[tap_index:tap_index + SEQ]
    gate_sig = jax.nn.sigmoid(conv_gate.astype(jnp.float32))
    grad_conv_value = (d_mixin * gate_sig).astype(jnp.bfloat16)
    grad_conv_gate = (d_mixin * conv_value.astype(jnp.float32) * gate_sig * (1.0 - gate_sig)).astype(jnp.bfloat16)
    return (grad_gate_weights, grad_up_weights, grad_down_weights, grad_out_weight, grad_conv_value, grad_conv_gate)
```

```python
import functools

import jax
import jax.numpy as jnp
from jax import lax
from jax.experimental import pallas as pl
from jax.experimental.pallas import tpu as pltpu
from jax.sharding import PartitionSpec as P

epsilon = 1e-06
MESH = pl.DeviceIdType.MESH
f32 = jnp.float32
bf16 = jnp.bfloat16


def contract_rows(left, right):
    return lax.dot_general(left, right, (((0,), (0,)), ((), ())), preferred_element_type=f32)


def contract_cols(left, right):
    return lax.dot_general(left, right, (((1,), (1,)), ((), ())), preferred_element_type=f32)


def loop(count, body):
    if count <= 8:
        for i in range(count):
            body(i)
    else:
        def step(i, carry):
            body(i)
            return carry
        lax.fori_loop(0, count, step, 0)


def remote(src, dst, send, recv, sp, tp):
    return pltpu.make_async_remote_copy(
        src_ref=src, dst_ref=dst, send_sem=send, recv_sem=recv,
        device_id={"sp": sp, "tp": tp}, device_id_type=MESH,
    )


def greet(sps, tps, sp, tp):
    barrier = pltpu.get_barrier_semaphore()

    def over_sp(d):
        pl.semaphore_signal(barrier, inc=1, device_id={"sp": (sp + d + 1) % sps, "tp": tp}, device_id_type=MESH)

    def over_tp(d):
        pl.semaphore_signal(barrier, inc=1, device_id={"sp": sp, "tp": (tp + d + 1) % tps}, device_id_type=MESH)

    loop(sps - 1, over_sp)
    loop(tps - 1, over_tp)
    pl.semaphore_wait(barrier, sps + tps - 2)


def dispatch_kernel(sps, tps, in_ref, out_ref, loc_sem, send_a, send_b, recv):
    sp, tp = lax.axis_index("sp"), lax.axis_index("tp")
    width = in_ref.shape[-1]

    def spot(s, t):
        return out_ref.at[:, s, :, pl.ds(pl.multiple_of(t * width, width), width)]

    own = pltpu.make_async_copy(in_ref.at[:, sp], spot(sp, tp), loc_sem)
    own.start()
    greet(sps, tps, sp, tp)

    def first(d, wait=False):
        to = (sp + d + 1) % sps
        copy = remote(in_ref.at[:, to], spot(sp, tp), send_a.at[d], recv.at[sp, tp], to, tp)
        copy.wait_send() if wait else copy.start()

    loop(sps - 1, first)

    def got(s, t):
        remote(spot(s, t), spot(s, t), send_a.at[0], recv.at[s, t], (sp + 1) % sps, tp).wait_recv()

    own.wait()
    if tps == 4:
        x, y = tp % 2, tp // 2
        xn, yn = y * 2 + (1 - x), (1 - y) * 2 + x
        diag = 3 - tp

        def direct(d, wait=False):
            s = (sp + sps - d) % sps
            for k, to in enumerate((xn, yn)):
                copy = remote(spot(s, tp), spot(s, tp), send_b.at[s, k], recv.at[s, tp], sp, to)
                copy.wait_send() if wait else copy.start()

        def relay(d, wait=False):
            s = (sp + sps - d) % sps
            odd = d % 2
            held = xn if odd == 0 else yn
            to = yn if odd == 0 else xn
            if not wait:
                got(s, held)
            copy = remote(spot(s, held), spot(s, held), send_b.at[s, 2], recv.at[s, held], sp, to)
            copy.wait_send() if wait else copy.start()
            if not wait:
                got(s, yn if odd == 0 else xn)

        assert sps <= 8
        direct(0)
        for d in range(1, sps):
            got((sp + sps - d) % sps, tp)
            direct(d)
            relay(d - 1)
        relay(sps - 1)
        for d in range(sps):
            got((sp + sps - d) % sps, diag)
        for d in range(sps):
            direct(d, True)
            relay(d, True)
    else:
        def spread(d, wait=False):
            s = (sp + sps - d) % sps

            def one(k):
                copy = remote(spot(s, tp), spot(s, tp), send_b.at[s, k], recv.at[s, tp], sp, (tp + k + 1) % tps)
                copy.wait_send() if wait else copy.start()

            loop(tps - 1, one)

        spread(0)

        def later(d):
            got((sp + sps - d - 1) % sps, tp)
            spread(d + 1)

        loop(sps - 1, later)
        loop(sps, lambda s: loop(tps - 1, lambda k: got(s, (tp + k + 1) % tps)))
        loop(sps, lambda d: spread(d, True))
    loop(sps - 1, lambda d: first(d, True))


def dispatch(send, sps, tps):
    parts, _, cap, width = send.shape
    return pl.pallas_call(
        functools.partial(dispatch_kernel, sps, tps),
        out_shape=jax.ShapeDtypeStruct((parts, sps, cap, width * tps), send.dtype),
        in_specs=[pl.BlockSpec(memory_space=pltpu.VMEM)],
        out_specs=pl.BlockSpec(memory_space=pltpu.VMEM),
        scratch_shapes=[
            pltpu.SemaphoreType.DMA,
            pltpu.SemaphoreType.DMA((sps,)),
            pltpu.SemaphoreType.DMA((sps, tps)),
            pltpu.SemaphoreType.DMA((sps, tps)),
        ],
        compiler_params=pltpu.CompilerParams(collective_id=0, has_side_effects=True),
        name="dispatch",
    )(send)


def combine_kernel(sps, tps, back_ref, comb_ref, act_ref, dn_ref, acts_ref, stage, sums, ret, total, part,
                   loc_sem, send_c, recv_c, send_r, recv_r, send_a, recv_a, send_g, recv_g):
    sp, tp = lax.axis_index("sp"), lax.axis_index("tp")
    width = ret.shape[-1]

    def cols(ref, t):
        return ref.at[:, pl.ds(pl.multiple_of(t * width, width), width)]

    own = pltpu.make_async_copy(act_ref, acts_ref.at[sp], loc_sem)
    own.start()
    greet(sps, tps, sp, tp)

    def reduce_send(d, wait=False):
        s = (sp + d + 1) % sps

        def one(k):
            to = (tp + k + 1) % tps
            copy = remote(cols(back_ref.at[s], to), stage.at[tp, s], send_r.at[s, k], recv_r.at[tp, s], sp, to)
            copy.wait_send() if wait else copy.start()

        loop(tps - 1, one)

    loop(sps, reduce_send)

    def act_send(d, wait=False):
        to = (sp + d + 1) % sps
        copy = remote(act_ref, acts_ref.at[sp], send_c.at[d], recv_c.at[sp], to, tp)
        copy.wait_send() if wait else copy.start()

    loop(sps - 1, act_send)

    def reduced(s):
        def take(k):
            t = (tp + k + 1) % tps
            remote(stage.at[t, s], stage.at[t, s], send_r.at[0, 0], recv_r.at[t, s], sp, t).wait_recv()

        loop(tps - 1, take)
        value = back_ref[s, :, pl.ds(pl.multiple_of(tp * width, width), width)].astype(f32)
        for k in range(tps - 1):
            value = value + stage[(tp + k + 1) % tps, s].astype(f32)
        return value.astype(bf16)

    def turn(d, wait=False):
        s = (sp + d + 1) % sps
        if not wait:
            sums[s] = reduced(s)
        copy = remote(sums.at[s], ret.at[sp], send_a.at[d], recv_a.at[sp], s, tp)
        copy.wait_send() if wait else copy.start()

    loop(sps - 1, turn)
    total[...] = jnp.dot(comb_ref[sp], reduced(sp), preferred_element_type=f32)

    def add(d):
        s = (sp + sps - d - 1) % sps
        remote(ret.at[s], ret.at[s], send_a.at[0], recv_a.at[s], s, tp).wait_recv()
        total[...] += jnp.dot(comb_ref[s], ret[s], preferred_element_type=f32)

    loop(sps - 1, add)
    part[...] = total[...].astype(bf16)

    def gather(k, wait=False):
        to = (tp + k + 1) % tps
        copy = remote(part, cols(dn_ref, tp), send_g.at[k], recv_g.at[tp], sp, to)
        copy.wait_send() if wait else copy.start()

    loop(tps - 1, gather)
    dn_ref[:, pl.ds(pl.multiple_of(tp * width, width), width)] = total[...].astype(bf16)

    def gathered(k):
        t = (tp + k + 1) % tps
        remote(part, cols(dn_ref, t), send_g.at[0], recv_g.at[t], sp, t).wait_recv()

    loop(tps - 1, gathered)

    def act_take(d):
        s = (sp + sps - d - 1) % sps
        remote(act_ref, acts_ref.at[s], send_c.at[0], recv_c.at[s], s, tp).wait_recv()

    loop(sps - 1, act_take)
    own.wait()
    loop(sps, lambda d: reduce_send(d, True))
    loop(sps - 1, lambda d: act_send(d, True))
    loop(sps - 1, lambda d: turn(d, True))
    loop(tps - 1, lambda k: gather(k, True))


def combine(back, comb, act, sps, tps):
    _, cap, model = back.shape
    tok, channels = act.shape
    width = model // tps
    dma = pltpu.SemaphoreType.DMA
    vm = pl.BlockSpec(memory_space=pltpu.VMEM)
    return pl.pallas_call(
        functools.partial(combine_kernel, sps, tps),
        out_shape=(
            jax.ShapeDtypeStruct((tok, model), bf16),
            jax.ShapeDtypeStruct((sps, tok, channels), bf16),
        ),
        in_specs=[vm] * 3,
        out_specs=(vm, vm),
        scratch_shapes=[
            pltpu.VMEM((tps, sps, cap, width), bf16),
            pltpu.VMEM((sps, cap, width), bf16),
            pltpu.VMEM((sps, cap, width), bf16),
            pltpu.VMEM((tok, width), f32),
            pltpu.VMEM((tok, width), bf16),
            dma,
            dma((sps,)),
            dma((sps,)),
            dma((sps, tps)),
            dma((tps, sps)),
            dma((sps,)),
            dma((sps,)),
            dma((tps,)),
            dma((tps,)),
        ],
        compiler_params=pltpu.CompilerParams(collective_id=1, has_side_effects=True),
        name="combine",
    )(back, comb, act)


def finish_kernel(sps, tps, halo, dm_ref, d_in_ref, norm_in_ref, rstd_ref, taps_ref, all_ref, mix_ref,
                  ext, part, parts, loc_sem, send_m, recv_m, send_s, recv_s, send_h, recv_h):
    sp, tp = lax.axis_index("sp"), lax.axis_index("tp")
    tok = d_in_ref.shape[0]
    channel_total = d_in_ref.shape[1] * tps
    own = pltpu.make_async_copy(dm_ref.at[sp], all_ref.at[sp], loc_sem)
    own.start()
    d_in = d_in_ref[...]
    norm_in = norm_in_ref[...]
    lane = lax.broadcasted_iota(jnp.int32, (tok, 128), 1)
    plain = jnp.sum(d_in, axis=1, keepdims=True)
    product = jnp.sum(d_in * norm_in, axis=1, keepdims=True)
    packed = jnp.where(lane == 0, plain, jnp.where(lane == 1, product, 0.0))
    mine = jnp.transpose(packed)[0:8]
    part[...] = mine
    greet(sps, tps, sp, tp)

    def sums_send(k, wait=False):
        to = (tp + k + 1) % tps
        copy = remote(part, parts.at[tp], send_s.at[k], recv_s.at[tp], sp, to)
        copy.wait_send() if wait else copy.start()

    loop(tps - 1, sums_send)

    def rows_send(d, wait=False):
        to = (sp + d + 1) % sps
        copy = remote(dm_ref.at[to], all_ref.at[sp], send_m.at[d], recv_m.at[sp], to, tp)
        copy.wait_send() if wait else copy.start()

    both = mine
    for k in range(tps - 1):
        t = (tp + k + 1) % tps
        remote(part, parts.at[t], send_s.at[0], recv_s.at[t], sp, t).wait_recv()
        both = both + parts[t]
    wide = jnp.transpose(jnp.concatenate([both] * 16, axis=0))
    plain = wide[:, 0:1] / channel_total
    product = wide[:, 1:2] / channel_total
    ext[0:tok, :] = rstd_ref[...] * (d_in - plain - norm_in * product)

    def halo_copy():
        return remote(ext.at[0:halo], ext.at[tok:tok + halo], send_h, recv_h, (sp + sps - 1) % sps, tp)

    @pl.when(sp > 0)
    def _():
        halo_copy().start()

    loop(sps - 1, rows_send)

    @pl.when(sp < sps - 1)
    def _():
        halo_copy().wait_recv()

    @pl.when(sp == sps - 1)
    def _():
        ext[tok:tok + halo, :] = jnp.zeros((halo, ext.shape[1]), f32)

    taps = taps_ref.shape[0]
    step = 32
    for base in range(0, tok, step):
        acc = taps_ref[0:1, :] * ext[base:base + step, :]
        for j in range(1, taps):
            acc = acc + taps_ref[j:j + 1, :] * ext[base + j:base + j + step, :]
        mix_ref[base:base + step, :] = acc

    def rows_take(d):
        s = (sp + sps - d - 1) % sps
        remote(dm_ref.at[s], all_ref.at[s], send_m.at[0], recv_m.at[s], s, tp).wait_recv()

    loop(sps - 1, rows_take)
    own.wait()

    @pl.when(sp > 0)
    def _():
        halo_copy().wait_send()

    loop(tps - 1, lambda k: sums_send(k, True))
    loop(sps - 1, lambda d: rows_send(d, True))


def finish(dm, d_in, norm_in, rstd, taps, sps, tps):
    tok, channels = d_in.shape
    halo = (taps.shape[0] + 7) // 8 * 8
    dma = pltpu.SemaphoreType.DMA
    vm = pl.BlockSpec(memory_space=pltpu.VMEM)
    return pl.pallas_call(
        functools.partial(finish_kernel, sps, tps, halo),
        out_shape=(
            jax.ShapeDtypeStruct(dm.shape, bf16),
            jax.ShapeDtypeStruct((tok, channels), f32),
        ),
        in_specs=[vm] * 5,
        out_specs=(vm, vm),
        scratch_shapes=[
            pltpu.VMEM((tok + halo, channels), f32),
            pltpu.VMEM((8, tok), f32),
            pltpu.VMEM((tps, 8, tok), f32),
            dma,
            dma((sps,)),
            dma((sps,)),
            dma((tps,)),
            dma((tps,)),
            dma,
            dma,
        ],
        compiler_params=pltpu.CompilerParams(collective_id=2, has_side_effects=True),
        name="finish",
    )(dm, d_in, norm_in, rstd, taps)


def local(
    cotangent,
    mixer_sum,
    ffn_gain,
    expert_ids,
    route_weight,
    gate_weights,
    up_weights,
    down_weights,
    out_weight,
    conv_output,
    norm_mean,
    norm_rstd,
    norm_gain,
    conv_taps,
    conv_value,
    conv_gate,
):
    tok_rows, model_width = cotangent.shape
    route_count = expert_ids.shape[1]
    sps = lax.axis_size("sp")
    tps = lax.axis_size("tp")
    capacity = 5 * route_count * tok_rows // (4 * sps)
    feature_share = model_width // tps
    feature_start = lax.axis_index("tp") * feature_share
    mixed_float = mixer_sum.astype(f32)
    row_rstd = lax.rsqrt(jnp.mean(mixed_float * mixed_float, axis=1, keepdims=True) + epsilon)
    mixer_hat = mixed_float * row_rstd

    experts = jnp.arange(sps, dtype=jnp.int32)
    named = [expert_ids[:, k][:, None] == experts[None, :] for k in range(route_count)]
    onehot = sum(n.astype(bf16) for n in named)
    order = jnp.arange(tok_rows, dtype=jnp.int32)
    lower = (order[:, None] > order[None, :]).astype(bf16)
    earlier = jnp.dot(lower, onehot, preferred_element_type=f32).astype(jnp.int32)
    place = jnp.where(onehot > 0, earlier, -1)
    weight = sum(jnp.where(named[k], route_weight[:, k][:, None], 0.0) for k in range(route_count))
    caps = jnp.arange(capacity, dtype=jnp.int32)
    place_t, weight_t = place.T, weight.T
    pick = place_t[:, None, :] == caps[None, :, None]
    slot_weight = jnp.sum(jnp.where(pick, weight_t[:, None, :], 0.0), axis=2)
    pick_b = pick.astype(bf16)
    comb = (place_t[:, :, None] == caps[None, None, :]).astype(bf16)

    mixer_part = lax.dynamic_slice_in_dim(mixer_sum, feature_start, feature_share, 1)
    gain_part = lax.dynamic_slice_in_dim(ffn_gain, feature_start, feature_share, 0)
    normed_part = (mixer_part.astype(f32) * row_rstd * gain_part).astype(bf16)
    cot_part = lax.dynamic_slice_in_dim(cotangent, feature_start, feature_share, 1)
    picks = pick_b.reshape(sps * capacity, tok_rows)
    picked = jnp.dot(picks, jnp.concatenate([normed_part, cot_part], axis=1), preferred_element_type=f32)
    send = jnp.stack([
        picked[:, :feature_share].astype(bf16),
        (picked[:, feature_share:] * slot_weight.reshape(-1)[:, None]).astype(bf16),
    ]).reshape(2, sps, capacity, feature_share)

    rows_all = dispatch(send, sps, tps)
    expert_rows = rows_all[0].reshape(-1, model_width)
    expert_cots = rows_all[1].reshape(-1, model_width)
    gate_mat = gate_weights[0]
    up_mat = up_weights[0]
    down_mat = down_weights[0]
    gate_pre = jnp.dot(expert_rows, gate_mat, preferred_element_type=f32)
    up_pre = jnp.dot(expert_rows, up_mat, preferred_element_type=f32)
    gate_sig = jax.nn.sigmoid(gate_pre)
    active = gate_pre * gate_sig
    hidden = (active * up_pre).astype(bf16)
    d_hidden = contract_cols(expert_cots, down_mat)
    d_gate = (d_hidden * up_pre * gate_sig * (1.0 + gate_pre * (1.0 - gate_sig))).astype(bf16)
    d_up = (d_hidden * active).astype(bf16)
    grad_down = contract_rows(hidden, expert_cots).astype(bf16)
    grad_gate = contract_rows(expert_rows, d_gate).astype(bf16)
    grad_up = contract_rows(expert_rows, d_up).astype(bf16)
    back_rows = (contract_cols(d_gate, gate_mat) + contract_cols(d_up, up_mat)).astype(bf16)

    norm_in = (conv_output.astype(f32) - norm_mean[:, None]) * norm_rstd[:, None]
    norm_scaled = norm_in * norm_gain
    norm_sig = jax.nn.sigmoid(norm_scaled)
    conv_act = (norm_scaled * norm_sig).astype(bf16)

    d_normed, acts_all = combine(back_rows.reshape(sps, capacity, model_width), comb, conv_act, sps, tps)
    d_hat = d_normed.astype(f32) * ffn_gain
    d_mixed = cotangent.astype(f32) + row_rstd * (
        d_hat - mixer_hat * jnp.mean(d_hat * mixer_hat, axis=1, keepdims=True)
    )
    d_mixed_b = d_mixed.astype(bf16)
    d_act = jnp.dot(d_mixed_b, out_weight, preferred_element_type=f32)
    d_in = d_act * norm_sig * (1.0 + norm_scaled * (1.0 - norm_sig)) * norm_gain
    blocks = d_mixed_b.reshape(tok_rows, sps, model_width // sps).transpose(1, 0, 2)
    dm_all, d_mixin = finish(blocks, d_in, norm_in, norm_rstd[:, None], conv_taps, sps, tps)
    grad_out_weight = contract_rows(
        dm_all.reshape(sps * tok_rows, -1), acts_all.reshape(sps * tok_rows, -1)
    )
    conv_sig = jax.nn.sigmoid(conv_gate.astype(f32))
    grad_conv_value = (d_mixin * conv_sig).astype(bf16)
    grad_conv_gate = (d_mixin * conv_value.astype(f32) * conv_sig * (1.0 - conv_sig)).astype(bf16)
    return (
        grad_gate[None],
        grad_up[None],
        grad_down[None],
        grad_out_weight,
        grad_conv_value,
        grad_conv_gate,
    )


def solution(mesh):
    return jax.shard_map(
        local,
        mesh=mesh,
        in_specs=(
            P("sp", None),
            P("sp", None),
            P(),
            P("sp", None),
            P("sp", None),
            P("sp", None, "tp"),
            P("sp", None, "tp"),
            P("sp", "tp", None),
            P(None, "tp"),
            P("sp", "tp"),
            P("sp"),
            P("sp"),
            P("tp"),
            P(None, "tp"),
            P("sp", "tp"),
            P("sp", "tp"),
        ),
        out_specs=(
            P("sp", None, "tp"),
            P("sp", None, "tp"),
            P("sp", "tp", None),
            P("sp", "tp"),
            P("sp", "tp"),
            P("sp", "tp"),
        ),
        check_vma=False,
    )
```
